256 devices in a mesh: rep: 2 (over z_hi), fs: 16 (over z_lo, x), tp: 8 (over y, core).
Axes of the slice: x: 4, y: 4, z: 8 (z_hi: 2, z_lo: 4; z = z_hi * 4 + z_lo), core: 2. Of those that a mesh axis runs over, the one named last changes fastest.
Arguments:
- tokens: bfloat16 [32768, 2048], P(('rep', 'fs'), 'tp'), may hold values from -6 to 6
- mix_gain: float32 [2048], replicated, may hold values from 0.1 to 1.9
- query_weight: bfloat16 [2048, 512], P('fs', 'tp'), may hold values from -0.125 to 0.125
- key_weight: bfloat16 [2048, 512], P('fs', 'tp'), may hold values from -0.125 to 0.125
- value_weight: bfloat16 [2048, 1024], P('fs', 'tp'), may hold values from -0.125 to 0.125
- gate_weight: bfloat16 [2048, 1024], P('fs', 'tp'), may hold values from -0.125 to 0.125
- out_weight: bfloat16 [1024, 2048], P('tp', 'fs'), may hold values from -0.1875 to 0.1875
- head_gain: float32 [8, 128], P('tp'), may hold values from 0.1 to 1.9
- ffn_gain: float32 [2048], replicated, may hold values from 0.1 to 1.9
- ffn_gate: bfloat16 [2048, 5632], P('fs', 'tp'), may hold values from -0.125 to 0.125
- ffn_up: bfloat16 [2048, 5632], P('fs', 'tp'), may hold values from -0.125 to 0.125
- ffn_down: bfloat16 [5632, 2048], P('tp', 'fs'), may hold values from -0.078125 to 0.078125
Outputs:
- layer_out: bfloat16 [32768, 2048], P(('rep', 'fs'), 'tp')
The draws below stay inside these ranges and needn't reach their ends.
All inputs are finite; a program needn't handle non-finite values.
Results may differ from the reference program's by a relative error of at most 0.03.
Values may be sent and summed in bfloat16 or wider, within the bound.
No kernel may reach another device: no remote copies, remote signals or barrier semaphores. Data moves between devices by JAX's collectives and lax.ppermute only.
A program may use at most 128 MiB of HBM per device.

```python
import jax
import jax.numpy as jnp
from jax import lax

D = 2048
HEADS = 8
DK = 64
DV = 128
FF = 5632
SEQ = 256
TOKENS = 32768
N_TP = 8


def levels(rng, extent, shards, least, largest):
    gain = 1.0
    for dim, parts in shards:
        steps = jax.random.uniform(jax.random.fold_in(jax.random.fold_in(rng, 6), dim), (parts,), jnp.float32, least / len(shards), largest / len(shards))
        gain = gain * jnp.repeat(jnp.exp(steps), extent[dim] // parts).reshape((-1,) + (1,) * (len(extent) - 1 - dim))
    return gain


def normal_values(key, extent, scale, most, shards=(), held_as=jnp.bfloat16):
    level = levels(key, extent, shards, -0.22, 0.18) if shards else 1.0
    values = jax.random.normal(key, extent, jnp.float32) * scale * level
    return jnp.minimum(jnp.maximum(values, -most), most).astype(held_as)


def setup_inputs(seed: int = 0) -> dict:
    seeds = jax.random.split(jax.random.key(seed), 13)
    return {
        "tokens": normal_values(seeds[0], (TOKENS, D), 1.0, 6.0, ((0, 32), (1, 8))),
        "mix_gain": jnp.clip(1.0 + 0.18 * jax.random.normal(seeds[1], (D,), jnp.float32), 0.1, 1.9),
        "query_weight": normal_values(seeds[2], (D, HEADS * DK), D ** -0.5, 0.125, ((0, 16), (1, 8))),
        "key_weight": normal_values(seeds[3], (D, HEADS * DK), D ** -0.5, 0.125, ((0, 16), (1, 8))),
        "value_weight": normal_values(seeds[4], (D, HEADS * DV), D ** -0.5, 0.125, ((0, 16), (1, 8))),
        "gate_weight": normal_values(seeds[5], (D, HEADS * DV), D ** -0.5, 0.125, ((0, 16), (1, 8))),
        "out_weight": normal_values(seeds[6], (HEADS * DV, D), (HEADS * DV) ** -0.5, 0.1875, ((0, 8), (1, 16))),
        "head_gain": jnp.clip(1.0 + 0.18 * jax.random.normal(seeds[7], (HEADS, DV), jnp.float32), 0.1, 1.9),
        "ffn_gain": jnp.clip(1.0 + 0.18 * jax.random.normal(seeds[8], (D,), jnp.float32), 0.1, 1.9),
        "ffn_gate": normal_values(seeds[9], (D, FF), D ** -0.5, 0.125, ((0, 16), (1, 8))),
        "ffn_up": normal_values(seeds[10], (D, FF), D ** -0.5, 0.125, ((0, 16), (1, 8))),
        "ffn_down": normal_values(seeds[11], (FF, D), FF ** -0.5, 0.078125, ((0, 8), (1, 16))),
    }


epsilon = 1e-06
rope_base = 10000.0

def norm_rows(values, gain_row):
    floats = values.astype(jnp.float32)
    scaled = floats * lax.rsqrt(lax.optimization_barrier(jnp.mean(floats * floats, axis=-1, keepdims=True)) + epsilon)
    return (scaled * gain_row).astype(jnp.bfloat16)

def rotate(values, positions):
    half_dim = values.shape[-1] // 2
    frequency = rope_base ** (-jnp.linspace(0.0, 1.0, half_dim, dtype=jnp.float32))
    angles = positions.astype(jnp.float32)[:, None] * frequency[None, :]
    cosine = jnp.cos(angles)[:, None, :]
    sine_part = jnp.sin(angles)[:, None, :]
    paired = values.reshape(values.shape[:-1] + (half_dim, 2))
    leading = paired[..., 0]
    trailing = paired[..., 1]
    turned = jnp.stack([leading * cosine - trailing * sine_part, leading * sine_part + trailing * cosine], axis=-1)
    return turned.reshape(values.shape)

def log_decay(head_index, total_heads):
    return jnp.log1p(-jnp.exp2(-5.0 - 4.0 * head_index.astype(jnp.float32) / (total_heads - 1)))

def split_sum(left, right):
    columns = left.shape[1] // N_TP
    summed = jnp.zeros((left.shape[0], right.shape[1]), jnp.float32)
    for segment in range(N_TP):
        partial_value = jnp.dot(left[:, segment * columns:(segment + 1) * columns], right[segment * columns:(segment + 1) * columns], preferred_element_type=jnp.float32).astype(jnp.bfloat16)
        summed = summed + lax.optimization_barrier(partial_value).astype(jnp.float32)
    return summed

def reference(tokens, mix_gain, query_weight, key_weight, value_weight, gate_weight, out_weight, head_gain, ffn_gain, ffn_gate, ffn_up, ffn_down):
    highest = lax.Precision.HIGHEST
    row_count = tokens.shape[0]
    normed = norm_rows(tokens, mix_gain)

    def project(weight):
        return jnp.dot(normed, weight, preferred_element_type=jnp.float32).astype(jnp.bfloat16)
    positions = jnp.arange(row_count, dtype=jnp.int32) % SEQ
    queries = rotate(project(query_weight).astype(jnp.float32).reshape(row_count, HEADS, DK), positions)
    key_rows = rotate(project(key_weight).astype(jnp.float32).reshape(row_count, HEADS, DK), positions) * DK ** (-0.5)
    value_rows = project(value_weight).astype(jnp.float32).reshape(row_count, HEADS, DV)
    gate_rows = project(gate_weight).astype(jnp.float32)
    decay_rates = log_decay(jnp.arange(HEADS, dtype=jnp.int32), HEADS)
    offsets = jnp.arange(SEQ, dtype=jnp.int32)
    distance = (offsets[:, None] - offsets[None, :]).astype(jnp.float32)
    decay_mask = jnp.where(distance[None] >= 0.0, jnp.exp(jnp.maximum(distance, 0.0)[None] * decay_rates[:, None, None]), 0.0)
    seq_count = row_count // SEQ

    def one_sequence(inputs):
        query_seq, key_seq, value_seq = inputs
        scores = jnp.einsum('ihd,jhd->hij', query_seq, key_seq, precision=highest) * decay_mask
        return jnp.einsum('hij,jhv->ihv', scores, value_seq, precision=highest)
    retained = lax.map(one_sequence, (queries.reshape(seq_count, SEQ, HEADS, DK), key_rows.reshape(seq_count, SEQ, HEADS, DK), value_rows.reshape(seq_count, SEQ, HEADS, DV)))
    retained = retained.reshape(row_count, HEADS, DV)
    center = lax.optimization_barrier(jnp.mean(retained, axis=-1, keepdims=True))
    spread = lax.optimization_barrier(jnp.mean(jnp.square(retained - center), axis=-1, keepdims=True))
    grouped = (retained - center) * lax.rsqrt(spread + epsilon) * head_gain[None]
    mixed = (grouped.reshape(row_count, HEADS * DV) * jax.nn.silu(gate_rows)).astype(jnp.bfloat16)
    residual = (tokens.astype(jnp.float32) + split_sum(mixed, out_weight)).astype(jnp.bfloat16)
    normed_ffn = norm_rows(residual, ffn_gain)
    gate_hidden = jnp.dot(normed_ffn, ffn_gate, preferred_element_type=jnp.float32)
    up_hidden = jnp.dot(normed_ffn, ffn_up, preferred_element_type=jnp.float32)
    hidden = (jax.nn.silu(gate_hidden) * up_hidden).astype(jnp.bfloat16)
    return (residual.astype(jnp.float32) + split_sum(hidden, ffn_down)).astype(jnp.bfloat16)
```

```python
import jax
import jax.numpy as jnp
import numpy as np
from jax import lax
from jax.experimental import pallas as pl
from jax.experimental.pallas import tpu as pltpu
from jax.sharding import Mesh
from jax.sharding import PartitionSpec as P

HEADS = 8
DK = 64
DV = 128
SEQ = 256
D = 2048
LANES = 128
NF = 16
EPS = 1e-06
ROPE_BASE = 10000.0


ANY = pl.BlockSpec(memory_space=pl.ANY)
VM = pl.BlockSpec(memory_space=pltpu.VMEM)
SM = pl.BlockSpec(memory_space=pltpu.SMEM)
BF = jnp.bfloat16
F32 = jnp.float32


def ring(size, shift):
    return [(i, (i + shift) % size) for i in range(size)]


def alternating(size):
    return [(i, (i + (2 if i % 2 == 0 else -2)) % size) for i in range(size)]


X_AXIS = ("x", 4)
Z_AXIS = (("rep", "z"), 8)
Y_AXIS = ("y", 4)


def from_offset(array, axis, offset):
    name, size = axis
    if offset == 2:
        pairs = ring(size, 2) if size == 4 else alternating(size)
    else:
        pairs = ring(size, -offset)
    return lax.ppermute(array, name, pairs)


def core_swap(array):
    return lax.ppermute(array, "c", [(0, 1), (1, 0)])


OFFSETS = (0, -1, 1, 2)


def gather_direct(piece, axis):
    return [piece] + [from_offset(piece, axis, o) for o in OFFSETS[1:]]


def gather_relayed(piece, axis):
    half = piece.shape[0] // 2
    below = from_offset(piece, axis, -1)
    above = from_offset(piece, axis, 1)
    first = from_offset(above[:half], axis, 1)
    second = from_offset(below[half:], axis, -1)
    return [piece, below, above, first, second]


def weights_everywhere(packed):
    half = packed.shape[0] // 2
    left = jnp.stack(gather_direct(packed[:half], X_AXIS))
    right = jnp.stack(gather_direct(packed[half:], Z_AXIS))
    mine = gather_relayed(left, Z_AXIS) + gather_relayed(right, X_AXIS)
    other = [core_swap(p) for p in mine]
    return mine, other


def block_moves(pos, half_rows):
    z, x = pos
    moves = []
    for side in range(2):
        for place, (offset, entries) in enumerate(
            ((0, range(4)), (-1, range(4)), (1, range(4)), (2, range(2)), (2, range(2, 4)))
        ):
            for entry, kept in enumerate(entries):
                inner = OFFSETS[kept]
                if side == 0:
                    block = ((z + offset) & 3) * 4 + ((x + inner) & 3)
                else:
                    block = ((z + inner) & 3) * 4 + ((x + offset) & 3)
                moves.append((side * 5 + place, entry, block, side * half_rows))
    return moves


def weight_copies(pos, core, groups, dest, sem, rows):
    copies = []
    for which, refs in enumerate(groups):
        owner = core if which == 0 else 1 - core
        for piece, entry, block, first in block_moves(pos, rows // 2):
            copies.append(
                pltpu.make_async_copy(
                    refs[piece].at[entry],
                    dest.at[owner, block, pl.ds(first, rows // 2)],
                    sem,
                )
            )
    return copies


def activation_copies(y, refs, dest, sem):
    copies = []
    for ref, offset in zip(refs, OFFSETS):
        column = pl.multiple_of(((y + offset) & 3) * 512, 512)
        copies.append(pltpu.make_async_copy(ref, dest.at[:, pl.ds(column, 512)], sem))
    return copies


def norm_in_place(acts, gain):
    rows = acts.shape[0]
    step = 64

    def one(i, carry):
        at = pl.ds(pl.multiple_of(i * step, step), step)
        floats = acts[at, :].astype(F32)
        scale = lax.rsqrt(jnp.mean(floats * floats, axis=-1, keepdims=True) + EPS)
        acts[at, :] = (floats * scale * gain[...]).astype(BF)
        return carry

    lax.fori_loop(0, rows // step, one, 0)


def mixer_body(
    place, rates, gain, head_gain, cosine, sine, *refs
):
    xs = refs[0:4]
    mine = refs[4:14]
    other = refs[14:24]
    outs = refs[24:28]
    acts, weights, mixed, sem, wsem = refs[28:]
    y, c, z, x = place[0], place[1], place[2], place[3]
    loads = activation_copies(y, xs, acts, sem)
    wloads = weight_copies((z, x), c, (mine, other), weights, wsem, 512)
    for copy in loads:
        copy.start()
    for copy in wloads:
        copy.start()
    for copy in loads:
        copy.wait()
    norm_in_place(acts, gain)
    for copy in wloads:
        copy.wait()
    rows = acts.shape[0]
    seqs = rows // SEQ
    lane = lax.broadcasted_iota(jnp.int32, (SEQ, LANES), 1)
    even = (lane & 1) == 0
    low = lane < DK
    gap = (
        lax.broadcasted_iota(jnp.int32, (SEQ, SEQ), 0)
        - lax.broadcasted_iota(jnp.int32, (SEQ, SEQ), 1)
    ).astype(F32)

    for s in range(2):
        mask = jnp.where(gap >= 0.0, jnp.exp(jnp.maximum(gap, 0.0) * rates[2 * y + s]), 0.0)
        wide = jnp.concatenate(
            [weights[s, :, k * LANES : (k + 1) * LANES, :].reshape(D, LANES) for k in range(3)],
            axis=1,
        )

        def one(i, carry, s=s, mask=mask, wide=wide):
            at = pl.ds(pl.multiple_of(i * SEQ, SEQ), SEQ)
            proj = jnp.dot(acts[at, :], wide, preferred_element_type=F32).astype(BF)
            both = proj[:, :LANES].astype(F32)
            values = proj[:, LANES : 2 * LANES]
            gate = proj[:, 2 * LANES :].astype(F32)
            swapped = jnp.where(even, pltpu.roll(both, LANES - 1, 1), pltpu.roll(both, 1, 1))
            turned = both * cosine[...] + swapped * sine[...]
            query = jnp.where(low, turned, 0.0)
            key = pltpu.roll(turned, DK, 1) * DK ** (-0.5)
            scores = lax.dot_general(
                query.astype(BF), key.astype(BF), (((1,), (1,)), ((), ())),
                preferred_element_type=F32,
            )
            retained = jnp.dot((scores * mask).astype(BF), values, preferred_element_type=F32)
            center = jnp.mean(retained, axis=-1, keepdims=True)
            off = retained - center
            spread = jnp.mean(off * off, axis=-1, keepdims=True)
            grouped = off * lax.rsqrt(spread + EPS) * head_gain[s : s + 1, :]
            mixed[at, s * DV : (s + 1) * DV] = (grouped * jax.nn.silu(gate)).astype(BF)
            return carry

        lax.fori_loop(0, seqs, one, 0)

    for d, out in enumerate(outs):
        chip = (y + OFFSETS[d]) & 3
        columns = [
            jnp.concatenate(
                [weights[s, chip * 4 + k, 384:512, :] for s in range(2)], axis=0
            )
            for k in range(4)
        ]
        out[...] = jnp.dot(
            mixed[...], jnp.concatenate(columns, axis=1), preferred_element_type=F32
        ).astype(BF)


def mixer(place, rates, gain, head_gain, cosine, sine, xs, mine, other):
    rows = xs[0].shape[0]
    return pl.pallas_call(
        mixer_body,
        out_shape=[jax.ShapeDtypeStruct((rows, 512), BF)] * 4,
        in_specs=[SM, SM, VM, VM, VM, VM] + [ANY] * 24,
        out_specs=[VM] * 4,
        scratch_shapes=[
            pltpu.VMEM((rows, D), BF),
            pltpu.VMEM((2, NF, 512, LANES), BF),
            pltpu.VMEM((rows, 2 * DV), BF),
            pltpu.SemaphoreType.DMA,
            pltpu.SemaphoreType.DMA,
        ],
        compiler_params=pltpu.CompilerParams(vmem_limit_bytes=40 * 2**20),
        cost_estimate=pl.CostEstimate(
            flops=2 * rows * D * 768 + 2 * rows * 256 * D, bytes_accessed=8 * 2**20, transcendentals=0
        ),
        name="mixer",
    )(place, rates, gain, head_gain, cosine, sine, *xs, *mine, *other)


PER_CORE = 704
GU_BLOCKS = 11
FFN_ROWS = 2112


def ffn_body(place, gain, *refs):
    xs = refs[0:4]
    mine = refs[4:14]
    other = refs[14:24]
    outs = refs[24:28]
    acts, weights, first, hidden, sem, wsem = refs[28:]
    y, c, z, x = place[0], place[1], place[2], place[3]
    loads = activation_copies(y, xs, acts, sem)
    wloads = weight_copies((z, x), c, (mine, other), weights, wsem, FFN_ROWS)
    for copy in loads:
        copy.start()
    for copy in wloads:
        copy.start()
    for copy in loads:
        copy.wait()
    norm_in_place(acts, gain)
    for copy in wloads:
        copy.wait()
    rows = acts.shape[0]

    def columns(j, carry):
        at = pl.ds(pl.multiple_of(j * LANES, LANES), LANES)
        wide = jnp.concatenate(
            [weights[s, :, at, :].reshape(D, LANES) for s in range(2)], axis=1
        )
        result = jnp.dot(acts[...], wide, preferred_element_type=F32)
        for s in range(2):
            first[s, j] = result[:, s * LANES : (s + 1) * LANES]
        return carry

    lax.fori_loop(0, GU_BLOCKS, columns, 0)
    step = 64

    def activate(i, carry):
        at = pl.ds(pl.multiple_of(i * step, step), step)
        for s in range(2):
            whole = jnp.concatenate([first[s, j, at, :] for j in range(GU_BLOCKS)], axis=1)
            hidden[s, at, :] = (jax.nn.silu(whole[:, :PER_CORE]) * whole[:, PER_CORE:]).astype(BF)
        return carry

    lax.fori_loop(0, rows // step, activate, 0)
    for d, out in enumerate(outs):
        chip = (y + OFFSETS[d]) & 3
        total = None
        for s in range(2):
            wide = jnp.concatenate(
                [weights[s, chip * 4 + k, 1408:2112, :] for k in range(4)], axis=1
            )
            part = jnp.dot(hidden[s], wide, preferred_element_type=F32)
            total = part if total is None else total + part
        out[...] = total.astype(BF)


def feed_forward(place, gain, xs, mine, other):
    rows = xs[0].shape[0]
    return pl.pallas_call(
        ffn_body,
        out_shape=[jax.ShapeDtypeStruct((rows, 512), BF)] * 4,
        in_specs=[SM, VM] + [ANY] * 24,
        out_specs=[VM] * 4,
        scratch_shapes=[
            pltpu.VMEM((rows, D), BF),
            pltpu.VMEM((2, NF, FFN_ROWS, LANES), BF),
            pltpu.VMEM((2, GU_BLOCKS, rows, LANES), F32),
            pltpu.VMEM((2, rows, PER_CORE), BF),
            pltpu.SemaphoreType.DMA,
            pltpu.SemaphoreType.DMA,
        ],
        compiler_params=pltpu.CompilerParams(vmem_limit_bytes=56 * 2**20),
        cost_estimate=pl.CostEstimate(
            flops=6 * rows * D * 1408, bytes_accessed=20 * 2**20, transcendentals=0
        ),
        name="feed_forward",
    )(place, gain, *xs, *mine, *other)


def pack_mixer_body(query, key, value, gate, out, packed):
    packed[0:128, :] = jnp.concatenate([query[...], key[...]], axis=1)
    packed[128:256, :] = value[...]
    packed[256:384, :] = gate[...]
    packed[384:512, :] = out[...]


def pack_ffn_body(gate, up, down, packed):
    both = jnp.concatenate([gate[...], up[...]], axis=1)
    for j in range(GU_BLOCKS):
        packed[j * 128 : (j + 1) * 128, :] = both[:, j * 128 : (j + 1) * 128]
    packed[1408:2112, :] = down[...]


def pack(body, rows, name, *arrays):
    return pl.pallas_call(
        body,
        out_shape=jax.ShapeDtypeStruct((rows, LANES), BF),
        in_specs=[VM] * len(arrays),
        out_specs=VM,
        name=name,
    )(*arrays)


def halves_in_order(c, own, received, axis):
    lower = jnp.where(c == 0, own, received)
    upper = jnp.where(c == 0, received, own)
    return jnp.concatenate([lower, upper], axis=axis)


def tables():
    frequency = ROPE_BASE ** (-np.linspace(0.0, 1.0, DK // 2))
    angles = np.arange(SEQ)[:, None] * frequency[None, :]
    cosine = np.repeat(np.cos(angles), 2, axis=1)
    sine = np.repeat(np.sin(angles), 2, axis=1) * np.tile([-1.0, 1.0], DK // 2)[None, :]
    return [np.tile(t, (1, 2)).astype(np.float32) for t in (cosine, sine)]


def reduce_pieces(pieces):
    total = pieces[0].astype(F32)
    for piece, offset in zip(pieces[1:], OFFSETS[1:]):
        total = total + from_offset(piece, Y_AXIS, 2 if offset == 2 else -offset).astype(F32)
    return total


def per_device(
    tokens,
    mix_gain,
    query_weight,
    key_weight,
    value_weight,
    gate_weight,
    out_weight,
    head_gain,
    ffn_gain,
    ffn_gate,
    ffn_up,
    ffn_down,
):
    y, c, z, x = (lax.axis_index(n) for n in ("y", "c", "z", "x"))
    place = jnp.stack([y, c, z, x]).astype(jnp.int32)
    cosine, sine = (jnp.asarray(t) for t in tables())
    rates = jnp.asarray(np.log1p(-np.exp2(-5.0 - 4.0 * np.arange(HEADS) / (HEADS - 1))), F32)
    half_rows = tokens.shape[0] // 2
    half_cols = tokens.shape[1]

    mixer_packed = pack(
        pack_mixer_body, 512, "pack_mixer", query_weight, key_weight, value_weight, gate_weight, out_weight
    )
    mixer_weights = weights_everywhere(mixer_packed)
    ffn_packed = pack(pack_ffn_body, FFN_ROWS, "pack_ffn", ffn_gate, ffn_up, ffn_down)
    ffn_weights = weights_everywhere(ffn_packed)
    heads_gain = halves_in_order(c, head_gain, core_swap(head_gain), 0)

    kept = lax.dynamic_slice_in_dim(tokens, c * half_rows, half_rows, 0)
    given = lax.dynamic_slice_in_dim(tokens, (1 - c) * half_rows, half_rows, 0)
    own = halves_in_order(c, kept, core_swap(given), 1)
    pieces = mixer(
        place, rates, mix_gain[None], heads_gain, cosine, sine, gather_direct(own, Y_AXIS), *mixer_weights
    )
    resid = (own.astype(F32) + reduce_pieces(pieces)).astype(BF)
    pieces = feed_forward(place, ffn_gain[None], gather_direct(resid, Y_AXIS), *ffn_weights)
    done = (resid.astype(F32) + reduce_pieces(pieces)).astype(BF)
    kept = lax.dynamic_slice_in_dim(done, c * half_cols, half_cols, 1)
    given = lax.dynamic_slice_in_dim(done, (1 - c) * half_cols, half_cols, 1)
    return halves_in_order(c, kept, core_swap(given), 0)


def solution(mesh):
    finer = Mesh(mesh.devices.reshape(2, 4, 4, 4, 2), ("rep", "z", "x", "y", "c"))
    fs, tp = ("z", "x"), ("y", "c")
    rows = ("rep", "z", "x")
    placed = (
        P(rows, tp), P(), P(fs, tp), P(fs, tp), P(fs, tp), P(fs, tp), P(tp, fs), P(tp, None), P(),
        P(fs, tp), P(fs, tp), P(tp, fs),
    )
    return jax.shard_map(
        per_device, mesh=finer, in_specs=placed, out_specs=P(rows, tp), check_vma=False
    )
```

```python
import jax
import jax.numpy as jnp
import numpy as np
from jax import lax
from jax.experimental import pallas as pl
from jax.experimental.pallas import tpu as pltpu
from jax.sharding import Mesh
from jax.sharding import PartitionSpec as P


HEADS = 8
DK = 64
DV = 128
SEQ = 256
D = 2048
LANES = 128
NF = 16
EPS = 1e-06
ROPE_BASE = 10000.0


ANY = pl.BlockSpec(memory_space=pl.ANY)
VM = pl.BlockSpec(memory_space=pltpu.VMEM)
SM = pl.BlockSpec(memory_space=pltpu.SMEM)
BF = jnp.bfloat16
F32 = jnp.float32

X_AXIS = ("x", 4)
Z_AXIS = (("rep", "z"), 8)
Y_AXIS = ("y", 4)
OFFSETS = (0, -1, 1, 2)


def ring(size, shift):
    return [(i, (i + shift) % size) for i in range(size)]


def alternating(size):
    return [(i, (i + (2 if i % 2 == 0 else -2)) % size) for i in range(size)]


def from_offset(array, axis, offset):
    name, size = axis
    if abs(offset) == 2:
        pairs = ring(size, 2) if size == 4 else alternating(size)
    else:
        pairs = ring(size, -offset)
    return lax.ppermute(array, name, pairs)


def core_swap(array):
    return lax.ppermute(array, "c", [(0, 1), (1, 0)])


def gather_direct(piece, axis):
    return [piece] + [from_offset(piece, axis, o) for k, o in enumerate(OFFSETS) if k]


def gather_relayed(piece, axis):
    half = piece.shape[0] // 2
    below = from_offset(piece, axis, -1)
    above = from_offset(piece, axis, 1)
    first = from_offset(above[:half], axis, 1)
    second = from_offset(below[half:], axis, -1)
    return [piece, below, above, first, second]


DIRECT = ((0, range(4)), (-1, range(4)), (1, range(4)), (2, range(4)))
RELAYED = ((0, range(4)), (-1, range(4)), (1, range(4)), (2, range(2)), (2, range(2, 4)))


def block_copies(pos, core, x_first, layout, mine, other, segments, sem):
    z, x = pos
    copies = []
    for refs, owner in ((mine, core), (other, 1 - core)):
        for ref, (outer, entries) in zip(refs, layout):
            for entry, kept in enumerate(entries):
                inner = OFFSETS[kept]
                dz, dx = (outer, inner) if x_first else (inner, outer)
                block = ((z + dz) & 3) * 4 + ((x + dx) & 3)
                for first, rows, target in segments(block, owner):
                    copies.append(
                        pltpu.make_async_copy(ref.at[entry, pl.ds(first, rows)], target, sem)
                    )
    return copies


def column_copies(y, refs, dest, sem):
    width = refs[0].shape[1]
    copies = []
    for ref, offset in zip(refs, OFFSETS):
        column = pl.multiple_of(((y + offset) & 3) * width, width)
        copies.append(pltpu.make_async_copy(ref, dest.at[:, pl.ds(column, width)], sem))
    return copies


def start_all(copies):
    for copy in copies:
        copy.start()


def wait_all(copies):
    for copy in copies:
        copy.wait()


def norm_rows(source, gain, dest):
    rows = source.shape[0]
    step = 64

    def one(i, carry):
        at = pl.ds(pl.multiple_of(i * step, step), step)
        floats = source[at, :].astype(F32)
        scale = lax.rsqrt(jnp.mean(floats * floats, axis=-1, keepdims=True) + EPS)
        dest[at, :] = (floats * scale * gain[...]).astype(BF)
        return carry

    lax.fori_loop(0, rows // step, one, 0)


TRANSPOSED = (((1,), (1,)), ((), ()))
M_ROWS = 384


def mixer_body(place, rates, gain, head_gain, cosine, sine, *refs):
    xs = refs[0:4]
    mine = refs[4:8]
    other = refs[8:12]
    mixed = refs[12]
    acts, weights, sem, wsem = refs[13:]
    y, c, z, x = place[0], place[1], place[2], place[3]
    loads = column_copies(y, xs, acts, sem)
    wloads = block_copies(
        (z, x), c, True, DIRECT, mine, other,
        lambda block, owner: [(0, M_ROWS, weights.at[owner, block])], wsem,
    )
    start_all(loads)
    start_all(wloads)
    wait_all(loads)
    norm_rows(acts, gain, acts)
    wait_all(wloads)
    rows = acts.shape[0]
    seqs = rows // SEQ
    lane = lax.broadcasted_iota(jnp.int32, (SEQ, LANES), 1)
    even = (lane & 1) == 0
    low = lane < DK
    gap = (
        lax.broadcasted_iota(jnp.int32, (SEQ, SEQ), 0)
        - lax.broadcasted_iota(jnp.int32, (SEQ, SEQ), 1)
    ).astype(F32)

    for s in range(2):
        mask = jnp.where(gap >= 0.0, jnp.exp(jnp.maximum(gap, 0.0) * rates[2 * y + s]), 0.0)
        turn = jnp.concatenate([weights[s, f, 0:128, :] for f in range(NF)], axis=1)
        wide = jnp.concatenate(
            [weights[s, :, k * LANES : (k + 1) * LANES, :].reshape(D, LANES) for k in (1, 2)],
            axis=1,
        )
        for i in range(seqs):
            at = slice(i * SEQ, (i + 1) * SEQ)
            both = lax.dot_general(acts[at, :], turn, TRANSPOSED, preferred_element_type=F32)
            both = both.astype(BF).astype(F32)
            proj = jnp.dot(acts[at, :], wide, preferred_element_type=F32).astype(BF)
            values = proj[:, :LANES]
            gate = proj[:, LANES:].astype(F32)
            swapped = jnp.where(even, pltpu.roll(both, LANES - 1, 1), pltpu.roll(both, 1, 1))
            turned = both * cosine[...] + swapped * sine[...]
            query = jnp.where(low, turned, 0.0)
            key = pltpu.roll(turned, DK, 1) * DK ** (-0.5)
            scores = lax.dot_general(
                query.astype(BF), key.astype(BF), TRANSPOSED, preferred_element_type=F32
            )
            retained = jnp.dot((scores * mask).astype(BF), values, preferred_element_type=F32)
            center = jnp.mean(retained, axis=-1, keepdims=True)
            off = retained - center
            spread = jnp.mean(off * off, axis=-1, keepdims=True)
            grouped = off * lax.rsqrt(spread + EPS) * head_gain[s : s + 1, :]
            mixed[at, s * DV : (s + 1) * DV] = (grouped * jax.nn.silu(gate)).astype(BF)


def mixer(place, rates, gain, head_gain, cosine, sine, xs, mine, other):
    rows = xs[0].shape[0]
    return pl.pallas_call(
        mixer_body,
        out_shape=jax.ShapeDtypeStruct((rows, 2 * DV), BF),
        in_specs=[SM, SM, VM, VM, VM, VM] + [ANY] * 12,
        out_specs=VM,
        scratch_shapes=[
            pltpu.VMEM((rows, D), BF),
            pltpu.VMEM((2, NF, M_ROWS, LANES), BF),
            pltpu.SemaphoreType.DMA,
            pltpu.SemaphoreType.DMA,
        ],
        compiler_params=pltpu.CompilerParams(vmem_limit_bytes=32 * 2**20),
        cost_estimate=pl.CostEstimate(
            flops=2 * rows * D * 768, bytes_accessed=5 * 2**20, transcendentals=0
        ),
        name="mixer",
    )(place, rates, gain, head_gain, cosine, sine, *xs, *mine, *other)


PER_CORE = 704
HIDDEN = 2 * PER_CORE


def ffn_body(place, gain, *refs):
    xs = refs[0:4]
    mixes = refs[4:8]
    b_mine, b_other = refs[8:13], refs[13:18]
    a_mine, a_other = refs[18:23], refs[23:28]
    base = refs[28]
    outs = refs[29:32]
    acts, mixed, normed, hidden, gate_up, outw, down, sems = refs[32:]
    y, c, z, x = place[0], place[1], place[2], place[3]

    def b_target(block, owner):
        at = owner * PER_CORE
        return [
            (0, PER_CORE, gate_up.at[block, pl.ds(at, PER_CORE)]),
            (PER_CORE, PER_CORE, gate_up.at[block, pl.ds(at + HIDDEN, PER_CORE)]),
        ]

    def a_target(block, owner):
        return [
            (k * DV, DV, outw.at[block, ((y + o) & 3) * 2 + owner])
            for k, o in enumerate(OFFSETS)
        ] + [(512, PER_CORE, down.at[block, pl.ds(owner * PER_CORE, PER_CORE)])]

    loads = column_copies(y, xs, acts, sems.at[0]) + column_copies(y, mixes, mixed, sems.at[0])
    a_loads = block_copies((z, x), c, True, RELAYED, a_mine, a_other, a_target, sems.at[1])
    b_loads = block_copies((z, x), c, False, RELAYED, b_mine, b_other, b_target, sems.at[2])
    start_all(loads)
    start_all(a_loads)
    start_all(b_loads)
    wait_all(loads)
    wait_all(a_loads)

    def project(n, carry):
        at = pl.ds(pl.multiple_of(n * 256, 256), 256)
        wide = jnp.concatenate(
            [outw[2 * n + k].reshape(HEADS * DV, LANES) for k in range(2)], axis=1
        )
        share = jnp.dot(mixed[...], wide, preferred_element_type=F32)
        acts[:, at] = (acts[:, at].astype(F32) + share).astype(BF)
        return carry

    lax.fori_loop(0, D // 256, project, 0)
    norm_rows(acts, gain, normed)
    wait_all(b_loads)

    def expand(j, carry):
        at = pl.ds(pl.multiple_of(j * LANES, LANES), LANES)
        up_at = pl.ds(pl.multiple_of(HIDDEN + j * LANES, LANES), LANES)
        wide = jnp.concatenate(
            [
                jnp.concatenate([gate_up[f, at, :], gate_up[f, up_at, :]], axis=0)
                for f in range(NF)
            ],
            axis=1,
        )
        both = lax.dot_general(normed[...], wide, TRANSPOSED, preferred_element_type=F32)
        hidden[:, at] = (jax.nn.silu(both[:, :LANES]) * both[:, LANES:]).astype(BF)
        return carry

    lax.fori_loop(0, HIDDEN // LANES, expand, 0)
    for d in range(4):
        chip = (y + OFFSETS[d]) & 3
        wide = jnp.concatenate([down[chip * 4 + k] for k in range(4)], axis=1)
        part = jnp.dot(hidden[...], wide, preferred_element_type=F32)
        if d == 0:
            own = acts[:, pl.ds(pl.multiple_of(y * 512, 512), 512)]
            base[...] = own.astype(F32) + part
        else:
            outs[d - 1][...] = part.astype(BF)


def feed_forward(place, gain, xs, mixes, b_both, a_both):
    rows = xs[0].shape[0]
    return pl.pallas_call(
        ffn_body,
        out_shape=[jax.ShapeDtypeStruct((rows, 512), F32)]
        + [jax.ShapeDtypeStruct((rows, 512), BF)] * 3,
        in_specs=[SM, VM] + [ANY] * 28,
        out_specs=[VM] * 4,
        scratch_shapes=[
            pltpu.VMEM((rows, D), BF),
            pltpu.VMEM((rows, HEADS * DV), BF),
            pltpu.VMEM((rows, D), BF),
            pltpu.VMEM((rows, HIDDEN), BF),
            pltpu.VMEM((NF, 2 * HIDDEN, LANES), BF),
            pltpu.VMEM((NF, HEADS, DV, LANES), BF),
            pltpu.VMEM((NF, HIDDEN, LANES), BF),
            pltpu.SemaphoreType.DMA((3,)),
        ],
        compiler_params=pltpu.CompilerParams(vmem_limit_bytes=48 * 2**20),
        cost_estimate=pl.CostEstimate(
            flops=6 * rows * D * HIDDEN, bytes_accessed=24 * 2**20, transcendentals=0
        ),
        name="ffn",
    )(place, gain, *xs, *mixes, *b_both[0], *b_both[1], *a_both[0], *a_both[1])


def halves_in_order(c, own, received, axis):
    lower = jnp.where(c == 0, own, received)
    upper = jnp.where(c == 0, received, own)
    return jnp.concatenate([lower, upper], axis=axis)


def tables():
    frequency = ROPE_BASE ** (-np.linspace(0.0, 1.0, DK // 2))
    angles = np.arange(SEQ)[:, None] * frequency[None, :]
    cosine = np.repeat(np.cos(angles), 2, axis=1)
    sine = np.repeat(np.sin(angles), 2, axis=1) * np.tile([-1.0, 1.0], DK // 2)[None, :]
    return [np.tile(t, (1, 2)).astype(np.float32) for t in (cosine, sine)]


def per_device(
    tokens,
    mix_gain,
    query_weight,
    key_weight,
    value_weight,
    gate_weight,
    out_weight,
    head_gain,
    ffn_gain,
    ffn_gate,
    ffn_up,
    ffn_down,
):
    y, c, z, x = (lax.axis_index(n) for n in ("y", "c", "z", "x"))
    place = jnp.stack([y, c, z, x]).astype(jnp.int32)
    cosine, sine = (jnp.asarray(t) for t in tables())
    rates = jnp.asarray(np.log1p(-np.exp2(-5.0 - 4.0 * np.arange(HEADS) / (HEADS - 1))), F32)
    half_rows = tokens.shape[0] // 2
    half_cols = tokens.shape[1]

    kept = lax.dynamic_slice_in_dim(tokens, c * half_rows, half_rows, 0)
    given = lax.dynamic_slice_in_dim(tokens, (1 - c) * half_rows, half_rows, 0)
    own = halves_in_order(c, kept, core_swap(given), 1)
    heads_gain = halves_in_order(c, head_gain, core_swap(head_gain), 0)

    packed = jnp.concatenate([query_weight.T, key_weight.T, value_weight, gate_weight], axis=0)
    row = jnp.stack(gather_direct(packed, X_AXIS))
    m_mine = gather_direct(row, Z_AXIS)
    m_other = [core_swap(p) for p in m_mine]

    packed = jnp.concatenate([ffn_gate.T, ffn_up.T], axis=0)
    column = jnp.stack(gather_direct(packed, Z_AXIS))
    b_mine = gather_relayed(column, X_AXIS)
    b_other = [core_swap(p) for p in b_mine]

    packed = jnp.concatenate(gather_direct(out_weight, Y_AXIS) + [ffn_down], axis=0)
    row = jnp.stack(gather_direct(packed, X_AXIS))
    a_mine = gather_relayed(row, Z_AXIS)
    a_other = [core_swap(p) for p in a_mine]

    xs = gather_direct(own, Y_AXIS)
    mixed = mixer(place, rates, mix_gain[None], heads_gain, cosine, sine, xs, m_mine, m_other)
    mixes = gather_direct(mixed, Y_AXIS)
    total, *shares = feed_forward(
        place, ffn_gain[None], xs, mixes, (b_mine, b_other), (a_mine, a_other)
    )
    for k, share in enumerate(shares):
        total = total + from_offset(share, Y_AXIS, -OFFSETS[k + 1]).astype(F32)
    done = total.astype(BF)
    kept = lax.dynamic_slice_in_dim(done, c * half_cols, half_cols, 1)
    given = lax.dynamic_slice_in_dim(done, (1 - c) * half_cols, half_cols, 1)
    return halves_in_order(c, kept, core_swap(given), 0)


def solution(mesh):
    finer = Mesh(mesh.devices.reshape(2, 4, 4, 4, 2), ("rep", "z", "x", "y", "c"))
    fs, tp = ("z", "x"), ("y", "c")
    rows = ("rep", "z", "x")
    placed = (
        P(rows, tp), P(), P(fs, tp), P(fs, tp), P(fs, tp), P(fs, tp), P(tp, fs), P(tp, None), P(),
        P(fs, tp), P(fs, tp), P(tp, fs),
    )
    return jax.shard_map(
        per_device, mesh=finer, in_specs=placed, out_specs=P(rows, tp), check_vma=False
    )
```

```python
import jax
import jax.numpy as jnp
import numpy as np
from jax import lax
from jax.experimental import pallas as pl
from jax.experimental.pallas import tpu as pltpu
from jax.sharding import Mesh
from jax.sharding import PartitionSpec as P


HEADS = 8
DK = 64
DV = 128
SEQ = 256
D = 2048
LANES = 128
NF = 16
EPS = 1e-06
ROPE_BASE = 10000.0


ANY = pl.BlockSpec(memory_space=pl.ANY)
VM = pl.BlockSpec(memory_space=pltpu.VMEM)
SM = pl.BlockSpec(memory_space=pltpu.SMEM)
BF = jnp.bfloat16
F32 = jnp.float32

X_AXIS = ("x", 4)
Z_AXIS = (("rep", "z"), 8)
Y_AXIS = ("y", 4)
OFFSETS = (0, -1, 1, 2)


def ring(size, shift):
    return [(i, (i + shift) % size) for i in range(size)]


def alternating(size):
    return [(i, (i + (2 if i % 2 == 0 else -2)) % size) for i in range(size)]


def from_offset(array, axis, offset):
    name, size = axis
    if abs(offset) == 2:
        pairs = ring(size, 2) if size == 4 else alternating(size)
    else:
        pairs = ring(size, -offset)
    return lax.ppermute(array, name, pairs)


def core_swap(array):
    return lax.ppermute(array, "c", [(0, 1), (1, 0)])


def gather_direct(piece, axis):
    return [piece] + [from_offset(piece, axis, o) for k, o in enumerate(OFFSETS) if k]


def gather_relayed(piece, axis):
    half = piece.shape[0] // 2
    below = from_offset(piece, axis, -1)
    above = from_offset(piece, axis, 1)
    first = from_offset(above[:half], axis, 1)
    second = from_offset(below[half:], axis, -1)
    return [piece, below, above, first, second]


DIRECT = ((0, range(4)), (-1, range(4)), (1, range(4)), (2, range(4)))
RELAYED = ((0, range(4)), (-1, range(4)), (1, range(4)), (2, range(2)), (2, range(2, 4)))


def block_copies(pos, core, x_first, layout, mine, other, segments, sem):
    z, x = pos
    copies = []
    for refs, owner in ((mine, core), (other, 1 - core)):
        for ref, (outer, entries) in zip(refs, layout):
            for entry, kept in enumerate(entries):
                inner = OFFSETS[kept]
                dz, dx = (outer, inner) if x_first else (inner, outer)
                block = ((z + dz) & 3) * 4 + ((x + dx) & 3)
                for first, rows, target in segments(block, owner):
                    copies.append(
                        pltpu.make_async_copy(ref.at[entry, pl.ds(first, rows)], target, sem)
                    )
    return copies


def column_copies(y, refs, dest, sem):
    width = refs[0].shape[1]
    copies = []
    for ref, offset in zip(refs, OFFSETS):
        column = pl.multiple_of(((y + offset) & 3) * width, width)
        copies.append(pltpu.make_async_copy(ref, dest.at[:, pl.ds(column, width)], sem))
    return copies


def start_all(copies):
    for copy in copies:
        copy.start()


def wait_all(copies):
    for copy in copies:
        copy.wait()


def norm_rows(source, gain, dest):
    rows = source.shape[0]
    step = 64

    def one(i, carry):
        at = pl.ds(pl.multiple_of(i * step, step), step)
        floats = source[at, :].astype(F32)
        scale = lax.rsqrt(jnp.mean(floats * floats, axis=-1, keepdims=True) + EPS)
        dest[at, :] = (floats * scale * gain[...]).astype(BF)
        return carry

    lax.fori_loop(0, rows // step, one, 0)


TRANSPOSED = (((1,), (1,)), ((), ()))
M_ROWS = 384


def mixer_body(place, rates, gain, head_gain, cosine, sine, *refs):
    xs = refs[0:4]
    mine = refs[4:8]
    other = refs[8:12]
    mixed = refs[12]
    acts, weights, sem, wsem = refs[13:]
    y, c, z, x = place[0], place[1], place[2], place[3]
    loads = column_copies(y, xs, acts, sem)
    wloads = block_copies(
        (z, x), c, True, DIRECT, mine, other,
        lambda block, owner: [(0, M_ROWS, weights.at[owner, block])], wsem,
    )
    start_all(loads)
    start_all(wloads)
    wait_all(loads)
    norm_rows(acts, gain, acts)
    wait_all(wloads)
    rows = acts.shape[0]
    seqs = rows // SEQ
    lane = lax.broadcasted_iota(jnp.int32, (SEQ, LANES), 1)
    even = (lane & 1) == 0
    low = lane < DK
    gap = (
        lax.broadcasted_iota(jnp.int32, (SEQ, SEQ), 0)
        - lax.broadcasted_iota(jnp.int32, (SEQ, SEQ), 1)
    ).astype(F32)

    for s in range(2):
        mask = jnp.where(gap >= 0.0, jnp.exp(jnp.maximum(gap, 0.0) * rates[2 * y + s]), 0.0)
        turn = jnp.concatenate([weights[s, f, 0:128, :] for f in range(NF)], axis=1)
        wide = jnp.concatenate(
            [weights[s, :, k * LANES : (k + 1) * LANES, :].reshape(D, LANES) for k in (1, 2)],
            axis=1,
        )
        for i in range(seqs):
            at = slice(i * SEQ, (i + 1) * SEQ)
            both = lax.dot_general(acts[at, :], turn, TRANSPOSED, preferred_element_type=F32)
            both = both.astype(BF).astype(F32)
            proj = jnp.dot(acts[at, :], wide, preferred_element_type=F32).astype(BF)
            values = proj[:, :LANES]
            gate = proj[:, LANES:].astype(F32)
            swapped = jnp.where(even, pltpu.roll(both, LANES - 1, 1), pltpu.roll(both, 1, 1))
            turned = both * cosine[...] + swapped * sine[...]
            query = jnp.where(low, turned, 0.0)
            key = pltpu.roll(turned, DK, 1) * DK ** (-0.5)
            scores = lax.dot_general(
                query.astype(BF), key.astype(BF), TRANSPOSED, preferred_element_type=F32
            )
            retained = jnp.dot((scores * mask).astype(BF), values, preferred_element_type=F32)
            center = jnp.mean(retained, axis=-1, keepdims=True)
            off = retained - center
            spread = jnp.mean(off * off, axis=-1, keepdims=True)
            grouped = off * lax.rsqrt(spread + EPS) * head_gain[s : s + 1, :]
            mixed[at, s * DV : (s + 1) * DV] = (grouped * jax.nn.silu(gate)).astype(BF)


def mixer(place, rates, gain, head_gain, cosine, sine, xs, mine, other):
    rows = xs[0].shape[0]
    return pl.pallas_call(
        mixer_body,
        out_shape=jax.ShapeDtypeStruct((rows, 2 * DV), BF),
        in_specs=[SM, SM, VM, VM, VM, VM] + [ANY] * 12,
        out_specs=VM,
        scratch_shapes=[
            pltpu.VMEM((rows, D), BF),
            pltpu.VMEM((2, NF, M_ROWS, LANES), BF),
            pltpu.SemaphoreType.DMA,
            pltpu.SemaphoreType.DMA,
        ],
        compiler_params=pltpu.CompilerParams(vmem_limit_bytes=32 * 2**20),
        cost_estimate=pl.CostEstimate(
            flops=2 * rows * D * 768, bytes_accessed=5 * 2**20, transcendentals=0
        ),
        name="mixer",
    )(place, rates, gain, head_gain, cosine, sine, *xs, *mine, *other)


PER_CORE = 704
HIDDEN = 2 * PER_CORE
UNIT = 64


def places(pos, x_first, layout, mine, other):
    z, x = pos
    result = []
    for p, (outer, entries) in enumerate(layout):
        for entry, kept in enumerate(entries):
            inner = OFFSETS[kept]
            dz, dx = (outer, inner) if x_first else (inner, outer)
            chip = (z + dz) & 3
            result.append((mine[p], other[p], entry, kept, chip, (x + dx) & 3))
    return result


def lanes(block):
    return pl.ds(pl.multiple_of(block * LANES, LANES), LANES)


def ffn_body(place, gain, *refs):
    xs = refs[0:4]
    mixes = refs[4:8]
    b_mine, b_other = refs[8:13], refs[13:18]
    a_mine, a_other = refs[18:23], refs[23:28]
    outs = refs[28:33]
    acts, mixed, normed, hidden, shares, sems = refs[33:]
    y, c, z, x = place[0], place[1], place[2], place[3]
    rows = acts.shape[0]
    loads = column_copies(y, xs, acts, sems.at[0])
    for ref, offset in zip(mixes, OFFSETS):
        chip = (y + offset) & 3
        for who in range(2):
            owner = c if who == 0 else 1 - c
            column = pl.multiple_of(chip * 256 + who * DV, DV)
            loads.append(
                pltpu.make_async_copy(
                    ref.at[:, lanes(owner)], mixed.at[:, pl.ds(column, DV)], sems.at[0]
                )
            )
    start_all(loads)
    wait_all(loads)
    b_places = places((z, x), False, RELAYED, b_mine, b_other)
    a_places = places((z, x), True, RELAYED, a_mine, a_other)

    for mine, other, entry, kept, chip, _ in a_places:
        at = lanes(chip * 4 + kept)
        wide = jnp.concatenate(
            [
                ref[entry, PER_CORE + k * DV : PER_CORE + (k + 1) * DV, :]
                for k in range(4)
                for ref in (mine, other)
            ],
            axis=0,
        )
        share = jnp.dot(mixed[...], wide, preferred_element_type=F32)
        acts[:, at] = (acts[:, at].astype(F32) + share).astype(BF)

    step = 64

    def norm(i, carry):
        at = pl.ds(pl.multiple_of(i * step, step), step)
        floats = acts[at, :].astype(F32)
        scale = lax.rsqrt(jnp.mean(floats * floats, axis=-1, keepdims=True) + EPS)
        for k, (_, _, _, _, zs, xb) in enumerate(b_places):
            here = lanes(zs * 4 + xb)
            normed[at, k * LANES : (k + 1) * LANES] = (
                acts[at, here].astype(F32) * scale * gain[:, here]
            ).astype(BF)
        return carry

    lax.fori_loop(0, rows // step, norm, 0)

    def expand(j, carry):
        gate_at = pl.ds(pl.multiple_of(j * UNIT, UNIT), UNIT)
        up_at = pl.ds(pl.multiple_of(PER_CORE + j * UNIT, UNIT), UNIT)
        wide = jnp.concatenate(
            [
                jnp.concatenate(
                    [ref[entry, at, :] for at in (gate_at, up_at) for ref in (mine, other)], axis=0
                )
                for mine, other, entry, _, _, _ in b_places
            ],
            axis=1,
        )
        both = lax.dot_general(normed[...], wide, TRANSPOSED, preferred_element_type=F32)
        hidden[:, lanes(j)] = (jax.nn.silu(both[:, :LANES]) * both[:, LANES:]).astype(BF)
        return carry

    lax.fori_loop(0, PER_CORE // UNIT, expand, 0)

    for first, second in zip(a_places[0::2], a_places[1::2]):
        wide = jnp.concatenate(
            [
                jnp.concatenate(
                    [
                        ref[entry, j * UNIT : (j + 1) * UNIT, :]
                        for j in range(PER_CORE // UNIT)
                        for ref in (mine, other)
                    ],
                    axis=0,
                )
                for mine, other, entry, _, _, _ in (first, second)
            ],
            axis=1,
        )
        part = jnp.dot(hidden[...], wide, preferred_element_type=F32).astype(BF)
        for k, (_, _, _, _, chip, xb) in enumerate((first, second)):
            shares[chip, :, lanes(xb)] = part[:, k * LANES : (k + 1) * LANES]

    stores = [
        pltpu.make_async_copy(shares.at[(y + offset) & 3], out, sems.at[1])
        for offset, out in zip(OFFSETS, outs[1:])
    ]
    stores.append(
        pltpu.make_async_copy(
            acts.at[:, pl.ds(pl.multiple_of(y * 512, 512), 512)], outs[0], sems.at[1]
        )
    )
    start_all(stores)
    wait_all(stores)


def feed_forward(place, gain, xs, mixes, b_both, a_both):
    rows = xs[0].shape[0]
    return pl.pallas_call(
        ffn_body,
        out_shape=[jax.ShapeDtypeStruct((rows, 512), BF)] * 5,
        in_specs=[SM, VM] + [ANY] * 8 + [VM] * 20,
        out_specs=[ANY] * 5,
        scratch_shapes=[
            pltpu.VMEM((rows, D), BF),
            pltpu.VMEM((rows, HEADS * DV), BF),
            pltpu.VMEM((rows, D), BF),
            pltpu.VMEM((rows, HIDDEN), BF),
            pltpu.VMEM((4, rows, 512), BF),
            pltpu.SemaphoreType.DMA((2,)),
        ],
        compiler_params=pltpu.CompilerParams(vmem_limit_bytes=VMEM_LIMIT),
        cost_estimate=pl.CostEstimate(
            flops=6 * rows * D * HIDDEN, bytes_accessed=24 * 2**20, transcendentals=0
        ),
        name="ffn",
    )(place, gain, *xs, *mixes, *b_both[0], *b_both[1], *a_both[0], *a_both[1])


VMEM_LIMIT = 40 * 2**20


def halves_in_order(c, own, received, axis):
    lower = jnp.where(c == 0, own, received)
    upper = jnp.where(c == 0, received, own)
    return jnp.concatenate([lower, upper], axis=axis)


def tables():
    frequency = ROPE_BASE ** (-np.linspace(0.0, 1.0, DK // 2))
    angles = np.arange(SEQ)[:, None] * frequency[None, :]
    cosine = np.repeat(np.cos(angles), 2, axis=1)
    sine = np.repeat(np.sin(angles), 2, axis=1) * np.tile([-1.0, 1.0], DK // 2)[None, :]
    return [np.tile(t, (1, 2)).astype(np.float32) for t in (cosine, sine)]


def per_device(
    tokens,
    mix_gain,
    query_weight,
    key_weight,
    value_weight,
    gate_weight,
    out_weight,
    head_gain,
    ffn_gain,
    ffn_gate,
    ffn_up,
    ffn_down,
):
    y, c, z, x = (lax.axis_index(n) for n in ("y", "c", "z", "x"))
    place = jnp.stack([y, c, z, x]).astype(jnp.int32)
    cosine, sine = (jnp.asarray(t) for t in tables())
    rates = jnp.asarray(np.log1p(-np.exp2(-5.0 - 4.0 * np.arange(HEADS) / (HEADS - 1))), F32)
    half_rows = tokens.shape[0] // 2
    half_cols = tokens.shape[1]

    kept = lax.dynamic_slice_in_dim(tokens, c * half_rows, half_rows, 0)
    given = lax.dynamic_slice_in_dim(tokens, (1 - c) * half_rows, half_rows, 0)
    own = halves_in_order(c, kept, core_swap(given), 1)
    heads_gain = halves_in_order(c, head_gain, core_swap(head_gain), 0)

    packed = jnp.concatenate([ffn_gate.T, ffn_up.T], axis=0)
    column = jnp.stack(gather_direct(packed, Z_AXIS))
    b_mine = gather_relayed(column, X_AXIS)
    b_other = [core_swap(p) for p in b_mine]

    packed = jnp.concatenate(
        [ffn_down, query_weight.T, key_weight.T, value_weight, gate_weight], axis=0
    )
    row = gather_direct(packed, X_AXIS)
    m_mine = gather_direct(jnp.stack([p[PER_CORE:] for p in row]), Z_AXIS)
    m_other = [core_swap(p) for p in m_mine]

    heads = lax.all_gather(out_weight, ("x", "y"), axis=0)
    heads = heads.reshape(4, 4 * DV, LANES)
    row = jnp.concatenate([jnp.stack([p[:PER_CORE] for p in row]), heads], axis=1)
    a_mine = gather_relayed(row, Z_AXIS)
    a_other = [core_swap(p) for p in a_mine]

    xs = gather_direct(own, Y_AXIS)
    mixed = mixer(place, rates, mix_gain[None], heads_gain, cosine, sine, xs, m_mine, m_other)
    mixes = gather_direct(mixed, Y_AXIS)
    resid, *shares = feed_forward(
        place, ffn_gain[None], xs, mixes, (b_mine, b_other), (a_mine, a_other)
    )
    total = resid.astype(F32) + shares[0].astype(F32)
    for k in range(1, 4):
        total = total + from_offset(shares[k], Y_AXIS, -OFFSETS[k]).astype(F32)
    done = total.astype(BF)
    kept = lax.dynamic_slice_in_dim(done, c * half_cols, half_cols, 1)
    given = lax.dynamic_slice_in_dim(done, (1 - c) * half_cols, half_cols, 1)
    return halves_in_order(c, kept, core_swap(given), 0)


def solution(mesh):
    finer = Mesh(mesh.devices.reshape(2, 4, 4, 4, 2), ("rep", "z", "x", "y", "c"))
    fs, tp = ("z", "x"), ("y", "c")
    rows = ("rep", "z", "x")
    placed = (
        P(rows, tp), P(), P(fs, tp), P(fs, tp), P(fs, tp), P(fs, tp), P(tp, fs), P(tp, None), P(),
        P(fs, tp), P(fs, tp), P(tp, fs),
    )
    return jax.shard_map(
        per_device, mesh=finer, in_specs=placed, out_specs=P(rows, tp), check_vma=False
    )
```

```python
import jax
import jax.numpy as jnp
import numpy as np
from jax import lax
from jax.experimental import pallas as pl
from jax.experimental.pallas import tpu as pltpu
from jax.sharding import Mesh
from jax.sharding import PartitionSpec as P


HEADS = 8
DK = 64
DV = 128
SEQ = 256
D = 2048
LANES = 128
NF = 16
EPS = 1e-06
ROPE_BASE = 10000.0


FAR = pl.BlockSpec(memory_space=pltpu.HBM)
VM = pl.BlockSpec(memory_space=pltpu.VMEM)
SM = pl.BlockSpec(memory_space=pltpu.SMEM)
BF = jnp.bfloat16
F32 = jnp.float32

X_AXIS = ("x", 4)
Z_AXIS = (("rep", "z"), 8)
Y_AXIS = ("y", 4)
OFFSETS = (0, -1, 1, 2)


def ring(size, shift):
    return [(i, (i + shift) % size) for i in range(size)]


def alternating(size):
    return [(i, (i + (2 if i % 2 == 0 else -2)) % size) for i in range(size)]


def from_offset(array, axis, offset):
    name, size = axis
    if abs(offset) == 2:
        pairs = ring(size, 2) if size == 4 else alternating(size)
    else:
        pairs = ring(size, -offset)
    return lax.ppermute(array, name, pairs)


def core_swap(array):
    return lax.ppermute(array, "c", [(0, 1), (1, 0)])


def gather_direct(piece, axis):
    return [piece] + [from_offset(piece, axis, o) for k, o in enumerate(OFFSETS) if k]


def gather_relayed(piece, axis):
    half = piece.shape[0] // 2
    below = from_offset(piece, axis, -1)
    above = from_offset(piece, axis, 1)
    first = from_offset(above[:half], axis, 1)
    second = from_offset(below[half:], axis, -1)
    return [piece, below, above, merge_halves(first, second)]


DIRECT = ((0, range(4)), (-1, range(4)), (1, range(4)), (2, range(4)))


TRANSPOSED = (((1,), (1,)), ((), ()))
M_ROWS = 384
STEP = 128


def lanes(block):
    return pl.ds(pl.multiple_of(block * LANES, LANES), LANES)


def mixer_body(place, rates, gain, table, *refs):
    xs, mine, other = refs[0:4], refs[4], refs[5]
    mixed, whole = refs[6:8]
    acts, scales, narrow, wide = refs[8:]
    y, c, z, x = place[0], place[1], place[2], place[3]
    for ref, offset in zip(xs, OFFSETS):
        whole[:, pl.ds(pl.multiple_of(((y + offset) & 3) * 512, 512), 512)] = ref[...]
    rows = whole.shape[0]

    def scale_gain(i, carry):
        at = pl.ds(pl.multiple_of(i * STEP, STEP), STEP)
        squares = jnp.zeros((STEP, LANES), F32)
        for k in range(NF):
            block = ((z + OFFSETS[k // 4]) & 3) * 4 + ((x + OFFSETS[k % 4]) & 3)
            floats = whole[at, lanes(block)].astype(F32)
            squares = squares + floats * floats
            acts[at, k * LANES : (k + 1) * LANES] = (floats * gain[:, lanes(block)]).astype(BF)
        total = jnp.sum(squares, axis=-1, keepdims=True)
        scales[at, :] = jnp.broadcast_to(lax.rsqrt(total / D + EPS), (STEP, LANES))
        return carry

    lax.fori_loop(0, rows // STEP, scale_gain, 0)

    turn = jnp.concatenate(
        [
            jnp.concatenate([ref[k * M_ROWS : k * M_ROWS + LANES] for ref in (mine, other)], axis=0)
            for k in range(NF)
        ],
        axis=1,
    )
    narrow[...] = lax.dot_general(acts[...], turn, TRANSPOSED, preferred_element_type=F32)
    straight = jnp.concatenate(
        [
            jnp.concatenate(
                [
                    ref[k * M_ROWS + part * LANES : k * M_ROWS + (part + 1) * LANES]
                    for ref in (mine, other)
                    for part in (1, 2)
                ],
                axis=1,
            )
            for k in range(NF)
        ],
        axis=0,
    )
    wide[...] = jnp.dot(acts[...], straight, preferred_element_type=F32)

    lane = lax.broadcasted_iota(jnp.int32, (SEQ, LANES), 1)
    even = (lane & 1) == 0
    low = lane < DK
    other_half = pltpu.roll(table[...], DK, 1)
    cosine = jnp.where(low, table[...], other_half)
    sine = jnp.where(low, other_half, table[...])
    gap = (
        lax.broadcasted_iota(jnp.int32, (SEQ, SEQ), 0)
        - lax.broadcasted_iota(jnp.int32, (SEQ, SEQ), 1)
    ).astype(F32)
    for who, (owner, ref) in enumerate(((c, mine), (1 - c, other))):
        terms = ref[NF * M_ROWS : NF * M_ROWS + 16].astype(F32)
        head_gain = terms[0:1] + terms[1:2] + terms[2:3]
        mask = jnp.where(gap >= 0.0, jnp.exp(jnp.maximum(gap, 0.0) * rates[2 * y + owner]), 0.0)
        for i in range(rows // SEQ):
            at = slice(i * SEQ, (i + 1) * SEQ)
            scale = scales[at, :]
            both = narrow[at, who * LANES : (who + 1) * LANES] * scale
            both = both.astype(BF).astype(F32)
            values = (wide[at, who * 256 : who * 256 + LANES] * scale).astype(BF)
            gate = (wide[at, who * 256 + LANES : (who + 1) * 256] * scale).astype(BF).astype(F32)
            swapped = jnp.where(even, pltpu.roll(both, LANES - 1, 1), pltpu.roll(both, 1, 1))
            turned = both * cosine + swapped * sine
            query = jnp.where(low, turned, 0.0)
            key = pltpu.roll(turned, DK, 1) * DK ** (-0.5)
            scores = lax.dot_general(
                query.astype(BF), key.astype(BF), TRANSPOSED, preferred_element_type=F32
            )
            retained = jnp.dot((scores * mask).astype(BF), values, preferred_element_type=F32)
            center = jnp.mean(retained, axis=-1, keepdims=True)
            off = retained - center
            spread = jnp.mean(off * off, axis=-1, keepdims=True)
            grouped = off * lax.rsqrt(spread + EPS) * head_gain
            mixed[at, who * DV : (who + 1) * DV] = (grouped * jax.nn.silu(gate)).astype(BF)


def mixer(place, rates, gain, table, xs, mine, other):
    rows = xs[0].shape[0]
    return pl.pallas_call(
        mixer_body,
        out_shape=[jax.ShapeDtypeStruct((rows, 2 * DV), BF), jax.ShapeDtypeStruct((rows, D), BF)],
        in_specs=[SM, SM] + [VM] * 8,
        out_specs=[VM, VM],
        scratch_shapes=[
            pltpu.VMEM((rows, D), BF),
            pltpu.VMEM((rows, LANES), F32),
            pltpu.VMEM((rows, 256), F32),
            pltpu.VMEM((rows, 512), F32),
        ],
        compiler_params=pltpu.CompilerParams(vmem_limit_bytes=20 * 2**20),
        cost_estimate=pl.CostEstimate(
            flops=2 * rows * D * 768, bytes_accessed=5 * 2**20, transcendentals=0
        ),
        name="mixer",
    )(place, rates, gain, table, *xs, mine, other)


PER_CORE = 704
HIDDEN = 2 * PER_CORE
UNIT = 64
PAIRS = 5
MOVED = 128
KEPT = PER_CORE - MOVED
B_ROWS = HIDDEN + MOVED


def quads(layout, mine, other):
    flat = []
    for ref, twin, (outer, entries) in zip(mine, other, layout):
        flat += [((ref, twin, entry), outer) for entry in range(len(entries))]
    for k in range(0, NF, 4):
        yield [entry for entry, _ in flat[k : k + 4]], flat[k][1]


def ffn_body(place, gain, whole, *refs):
    nb, na = len(B_LAYOUT), len(A_LAYOUT)
    mixes, refs = refs[0:4], refs[4:]
    b_mine, b_other, refs = refs[:nb], refs[nb : 2 * nb], refs[2 * nb :]
    a_mine, a_other, refs = refs[:na], refs[na : 2 * na], refs[2 * na :]
    own, *outs = refs[:7]
    resid, mixed, acts, hidden, shares, scales, squares = refs[7:]
    y, z, x = place[0], place[2], place[3]
    rows = whole.shape[0]
    for d, ref in enumerate(mixes):
        mixed[:, d * 256 : (d + 1) * 256] = ref[...]

    def columns(group, segments):
        return jnp.concatenate(
            [
                jnp.concatenate(
                    [ref[entry, at, :] for at in segments for ref in (mine, other)], axis=0
                )
                for mine, other, entry in group
            ],
            axis=1,
        )

    for group, outer in quads(A_LAYOUT, a_mine, a_other):
        wide = columns(group, [slice(KEPT + k * DV, KEPT + (k + 1) * DV) for k in range(4)])
        share = jnp.dot(mixed[...], wide, preferred_element_type=F32)
        for e, inner in enumerate(OFFSETS):
            at = lanes(((z + outer) & 3) * 4 + ((x + inner) & 3))
            rounded = (
                whole[:, at].astype(F32) + share[:, e * LANES : (e + 1) * LANES]
            ).astype(BF)
            resid[:, at] = rounded
            floats = rounded.astype(F32)
            k = e * 4 + OFFSETS.index(outer)
            acts[:, k * LANES : (k + 1) * LANES] = (floats * gain[:, at]).astype(BF)
            if e == 0 and outer == 0:
                squares[...] = floats * floats
            else:
                squares[...] += floats * floats

    total = jnp.sum(squares[...], axis=-1, keepdims=True)
    scales[...] = jnp.broadcast_to(lax.rsqrt(total / D + EPS), (rows, LANES))
    order = []
    for mine, other, (outer, entries) in zip(b_mine, b_other, B_LAYOUT):
        order += [(mine, other, entry) for entry in range(len(entries))]

    def multiply(j, units):
        width = units * UNIT
        gate_at = pl.ds(pl.multiple_of(j * UNIT, UNIT), width)
        up_at = pl.ds(pl.multiple_of(PER_CORE + j * UNIT, UNIT), width)
        wide = jnp.concatenate(
            [
                jnp.concatenate(
                    [ref[entry, at, :] for at in (gate_at, up_at) for ref in (mine, other)], axis=0
                )
                for mine, other, entry in order
            ],
            axis=1,
        )
        return lax.dot_general(acts[...], wide, TRANSPOSED, preferred_element_type=F32)

    def expand(i, carry):
        both = multiply(2 * i, 2)
        for k in range(2):
            gate = both[:, k * LANES : (k + 1) * LANES] * scales[...]
            up = both[:, 256 + k * LANES : 256 + (k + 1) * LANES] * scales[...]
            hidden[:, lanes(2 * i + k)] = (jax.nn.silu(gate) * up).astype(BF)
        return carry

    lax.fori_loop(0, PAIRS, expand, 0)
    both = multiply(2 * PAIRS, 1)
    gate, up = both[:, :LANES] * scales[...], both[:, LANES:] * scales[...]
    hidden[:, PAIRS * 256 :] = (jax.nn.silu(gate) * up).astype(BF)

    moved = [slice(HIDDEN, B_ROWS)]
    segments = [slice(2 * UNIT * i, 2 * UNIT * (i + 1)) for i in range(PAIRS - 1)]
    segments.append(slice(2 * UNIT * (PAIRS - 1), KEPT))
    for p, (group, outer) in enumerate(quads(A_LAYOUT, a_mine, a_other)):
        twins = [order[e * 4 + p] for e in range(4)]
        wide = jnp.concatenate([columns(twins, moved), columns(group, segments)], axis=0)
        part = jnp.dot(hidden[...], wide, preferred_element_type=F32).astype(BF)
        for e, inner in enumerate(OFFSETS):
            shares[(z + outer) & 3, :, lanes((x + inner) & 3)] = part[:, e * LANES : (e + 1) * LANES]

    half = rows // 2
    for (offset, first), out in zip(PIECES, outs):
        out[...] = shares[(y + offset) & 3, first * half : (first + 1) * half]
    mine = pl.ds(pl.multiple_of(y * 512, 512), 512)
    own[...] = resid[:, mine].astype(F32) + shares[y].astype(F32)


def feed_forward(place, gain, whole, mixes, b_both, a_both):
    rows = whole.shape[0]
    weights = [*b_both[0], *b_both[1], *a_both[0], *a_both[1]]
    return pl.pallas_call(
        ffn_body,
        out_shape=[jax.ShapeDtypeStruct((rows, 512), F32)]
        + [jax.ShapeDtypeStruct((rows // 2, 512), BF)] * 6,
        in_specs=[SM] + [VM] * (6 + len(weights)),
        out_specs=[VM] * 7,
        scratch_shapes=[
            pltpu.VMEM((rows, D), BF),
            pltpu.VMEM((rows, HEADS * DV), BF),
            pltpu.VMEM((rows, D), BF),
            pltpu.VMEM((rows, HIDDEN), BF),
            pltpu.VMEM((4, rows, 512), BF),
            pltpu.VMEM((rows, LANES), F32),
            pltpu.VMEM((rows, LANES), F32),
        ],
        compiler_params=pltpu.CompilerParams(vmem_limit_bytes=VMEM_LIMIT),
        cost_estimate=pl.CostEstimate(
            flops=6 * rows * D * HIDDEN, bytes_accessed=24 * 2**20, transcendentals=0
        ),
        name="ffn",
    )(place, gain, whole, *mixes, *weights)


PIECES = ((2, 0), (2, 1), (1, 0), (1, 1), (-1, 0), (-1, 1))
B_LAYOUT = DIRECT
A_LAYOUT = DIRECT
VMEM_LIMIT = 20 * 2**20


def join_body(place, tokens, received, own, sem):
    half, cols = received.shape
    c = place[1]
    copy = pltpu.make_async_copy(
        tokens.at[pl.ds(pl.multiple_of(c * half, half), half)],
        own.at[:, pl.ds(pl.multiple_of(c * cols, cols), cols)],
        sem,
    )
    copy.start()
    own[:, pl.ds(pl.multiple_of((1 - c) * cols, cols), cols)] = received[...]
    copy.wait()


def join(place, tokens, received):
    half, cols = received.shape
    return pl.pallas_call(
        join_body,
        out_shape=jax.ShapeDtypeStruct((half, 2 * cols), BF),
        in_specs=[SM, FAR, VM],
        out_specs=VM,
        scratch_shapes=[pltpu.SemaphoreType.DMA],
        compiler_params=pltpu.CompilerParams(vmem_limit_bytes=4 * 2**20),
        name="join",
    )(place, tokens, received)


def stack(pieces, parts):
    total = sum(rows for _, _, rows in parts(0))

    def body(*refs):
        *ins, out = refs
        for k in range(4):
            row = 0
            for source, first, rows in parts(k):
                out[k, row : row + rows, :] = ins[source][first : first + rows, :]
                row += rows

    return pl.pallas_call(
        body,
        out_shape=jax.ShapeDtypeStruct((4, total, LANES), BF),
        in_specs=[VM] * len(pieces),
        out_specs=VM,
        compiler_params=pltpu.CompilerParams(vmem_limit_bytes=4 * 2**20),
    )(*pieces)


def merge_mixer_body(gain, *refs):
    *pieces, out = refs
    for k in range(NF):
        out[k * M_ROWS : (k + 1) * M_ROWS, :] = pieces[k // 4][k % 4]
    rest = gain[...]
    terms = []
    for _ in range(3):
        terms.append(rest.astype(BF))
        rest = rest - terms[-1].astype(F32)
    terms.append(jnp.zeros((13, LANES), BF))
    out[NF * M_ROWS :, :] = jnp.concatenate([t.astype(F32) for t in terms], axis=0).astype(BF)


def merge_mixer(gain, pieces):
    return pl.pallas_call(
        merge_mixer_body,
        out_shape=jax.ShapeDtypeStruct((NF * M_ROWS + 16, LANES), BF),
        in_specs=[VM] * 5,
        out_specs=VM,
        compiler_params=pltpu.CompilerParams(vmem_limit_bytes=4 * 2**20),
        name="merge_mixer",
    )(gain, *pieces)


def merge_halves_body(first, second, out):
    out[0:2] = first[...]
    out[2:4] = second[...]


def merge_halves(first, second):
    return pl.pallas_call(
        merge_halves_body,
        out_shape=jax.ShapeDtypeStruct((4, *first.shape[1:]), BF),
        in_specs=[VM] * 2,
        out_specs=VM,
        compiler_params=pltpu.CompilerParams(vmem_limit_bytes=4 * 2**20),
    )(first, second)


def halves_in_order(c, own, received, axis):
    lower = jnp.where(c == 0, own, received)
    upper = jnp.where(c == 0, received, own)
    return jnp.concatenate([lower, upper], axis=axis)


def rotation_table():
    frequency = ROPE_BASE ** (-np.linspace(0.0, 1.0, DK // 2))
    angles = np.repeat(np.arange(SEQ)[:, None] * frequency[None, :], 2, axis=1)
    signs = np.tile([-1.0, 1.0], DK // 2)[None, :]
    return np.concatenate([np.cos(angles), np.sin(angles) * signs], axis=1).astype(np.float32)


def per_device(
    tokens,
    mix_gain,
    query_weight,
    key_weight,
    value_weight,
    gate_weight,
    out_weight,
    head_gain,
    ffn_gain,
    ffn_gate,
    ffn_up,
    ffn_down,
):
    y, c, z, x = (lax.axis_index(n) for n in ("y", "c", "z", "x"))
    place = jnp.stack([y, c, z, x]).astype(jnp.int32)
    table = jnp.asarray(rotation_table())
    rates = jnp.asarray(np.log1p(-np.exp2(-5.0 - 4.0 * np.arange(HEADS) / (HEADS - 1))), F32)
    half_cols = tokens.shape[1]

    b_pack = jnp.concatenate([ffn_gate.T, ffn_up.T, ffn_down[:MOVED]], axis=0)
    half = tokens.shape[0] // 2
    given = lax.dynamic_slice_in_dim(tokens, (1 - c) * half, half, 0)
    x_pack = jnp.concatenate([query_weight.T, key_weight.T, value_weight, gate_weight], axis=0)
    x_pack = jnp.concatenate([ffn_down[MOVED:], lax.optimization_barrier(x_pack), out_weight], axis=0)
    own = join(place, tokens, core_swap(given))

    column = stack(gather_direct(b_pack, Z_AXIS), lambda k: [(k, 0, B_ROWS)])
    b_mine = gather_relayed(column, X_AXIS)
    b_other = [core_swap(p) for p in b_mine]

    row = gather_direct(x_pack, X_AXIS)
    m_mine = gather_direct(stack(row, lambda k: [(k, KEPT, M_ROWS)]), Z_AXIS)
    m_mine = merge_mixer(head_gain, m_mine)
    m_other = core_swap(m_mine)

    heads = stack(row, lambda k: [(k, KEPT + M_ROWS, DV)]).reshape(4 * DV, LANES)
    heads = gather_direct(heads, Y_AXIS)
    row = stack([*row, *heads], lambda k: [(k, 0, KEPT)] + [(4 + d, k * DV, DV) for d in range(4)])
    a_mine = gather_relayed(row, Z_AXIS)
    a_other = [core_swap(p) for p in a_mine]

    xs = gather_direct(own, Y_AXIS)
    mixed, whole = mixer(
        place, rates, mix_gain[None], table, xs, m_mine, m_other
    )
    mixes = gather_direct(mixed, Y_AXIS)
    total, far_top, far_low, up_top, up_low, down_top, down_low = feed_forward(
        place, ffn_gain[None], whole, mixes, (b_mine, b_other), (a_mine, a_other)
    )
    far_top = from_offset(far_top, Y_AXIS, -1)
    far_low = from_offset(far_low, Y_AXIS, 1)
    near_low = from_offset(up_low, Y_AXIS, -1)
    near_top = from_offset(down_top, Y_AXIS, 1)
    up_top = (up_top.astype(F32) + far_top.astype(F32)).astype(BF)
    down_low = (down_low.astype(F32) + far_low.astype(F32)).astype(BF)
    top = near_top.astype(F32) + from_offset(up_top, Y_AXIS, -1).astype(F32)
    low = near_low.astype(F32) + from_offset(down_low, Y_AXIS, 1).astype(F32)
    total = total + jnp.concatenate([top, low], axis=0)
    done = total.astype(BF)
    kept = lax.dynamic_slice_in_dim(done, c * half_cols, half_cols, 1)
    given = lax.dynamic_slice_in_dim(done, (1 - c) * half_cols, half_cols, 1)
    return halves_in_order(c, kept, core_swap(given), 0)


def solution(mesh):
    finer = Mesh(mesh.devices.reshape(2, 4, 4, 4, 2), ("rep", "z", "x", "y", "c"))
    fs, tp = ("z", "x"), ("y", "c")
    rows = ("rep", "z", "x")
    placed = (
        P(rows, tp), P(), P(fs, tp), P(fs, tp), P(fs, tp), P(fs, tp), P(tp, fs), P(tp, None), P(),
        P(fs, tp), P(fs, tp), P(tp, fs),
    )
    return jax.shard_map(
        per_device, mesh=finer, in_specs=placed, out_specs=P(rows, tp), check_vma=False
    )
```

```python
import jax
import jax.numpy as jnp
import numpy as np
from jax import lax
from jax.experimental import pallas as pl
from jax.experimental.pallas import tpu as pltpu
from jax.sharding import Mesh
from jax.sharding import PartitionSpec as P


HEADS = 8
DK = 64
DV = 128
SEQ = 256
D = 2048
LANES = 128
NF = 16
EPS = 1e-06
ROPE_BASE = 10000.0


FAR = pl.BlockSpec(memory_space=pltpu.HBM)
VM = pl.BlockSpec(memory_space=pltpu.VMEM)
SM = pl.BlockSpec(memory_space=pltpu.SMEM)
BF = jnp.bfloat16
F32 = jnp.float32

X_AXIS = ("x", 4)
Z_AXIS = (("rep", "z"), 8)
Y_AXIS = ("y", 4)
OFFSETS = (0, -1, 1, 2)


def ring(size, shift):
    return [(i, (i + shift) % size) for i in range(size)]


def alternating(size):
    return [(i, (i + (2 if i % 2 == 0 else -2)) % size) for i in range(size)]


def from_offset(array, axis, offset):
    name, size = axis
    if abs(offset) == 2:
        pairs = ring(size, 2) if size == 4 else alternating(size)
    else:
        pairs = ring(size, -offset)
    return lax.ppermute(array, name, pairs)


def core_swap(array):
    return lax.ppermute(array, "c", [(0, 1), (1, 0)])


def gather_direct(piece, axis):
    return [piece] + [from_offset(piece, axis, o) for k, o in enumerate(OFFSETS) if k]


def gather_relayed(piece, axis):
    half = piece.shape[0] // 2
    below = from_offset(piece, axis, -1)
    above = from_offset(piece, axis, 1)
    above_half, below_half = above[:half], below[half:]
    first = from_offset(above_half, axis, 1)
    second = from_offset(below_half, axis, -1)
    return [piece, below, above, merge_halves(first, second)]


DIRECT = ((0, range(4)), (-1, range(4)), (1, range(4)), (2, range(4)))


TRANSPOSED = (((1,), (1,)), ((), ()))
M_ROWS = 384
STEP = 128


def lanes(block):
    return pl.ds(pl.multiple_of(block * LANES, LANES), LANES)


def mixer_body(place, rates, gain, table, *refs):
    xs, mine, other = refs[0:4], refs[4], refs[5]
    mixed, whole = refs[6:8]
    acts, scales, narrow, wide = refs[8:]
    y, c, z, x = place[0], place[1], place[2], place[3]
    for ref, offset in zip(xs, OFFSETS):
        whole[:, pl.ds(pl.multiple_of(((y + offset) & 3) * 512, 512), 512)] = ref[...]
    rows = whole.shape[0]

    def scale_gain(i, carry):
        at = pl.ds(pl.multiple_of(i * STEP, STEP), STEP)
        squares = jnp.zeros((STEP, LANES), F32)
        for k in range(NF):
            block = ((z + OFFSETS[k // 4]) & 3) * 4 + ((x + OFFSETS[k % 4]) & 3)
            floats = whole[at, lanes(block)].astype(F32)
            squares = squares + floats * floats
            acts[at, k * LANES : (k + 1) * LANES] = (floats * gain[:, lanes(block)]).astype(BF)
        total = jnp.sum(squares, axis=-1, keepdims=True)
        scales[at, :] = jnp.broadcast_to(lax.rsqrt(total / D + EPS), (STEP, LANES))
        return carry

    lax.fori_loop(0, rows // STEP, scale_gain, 0)

    turn = jnp.concatenate(
        [
            jnp.concatenate([ref[k * M_ROWS : k * M_ROWS + LANES] for ref in (mine, other)], axis=0)
            for k in range(NF)
        ],
        axis=1,
    )
    narrow[...] = lax.dot_general(acts[...], turn, TRANSPOSED, preferred_element_type=F32)
    straight = jnp.concatenate(
        [
            jnp.concatenate(
                [
                    ref[k * M_ROWS + part * LANES : k * M_ROWS + (part + 1) * LANES]
                    for ref in (mine, other)
                    for part in (1, 2)
                ],
                axis=1,
            )
            for k in range(NF)
        ],
        axis=0,
    )
    wide[...] = jnp.dot(acts[...], straight, preferred_element_type=F32)

    lane = lax.broadcasted_iota(jnp.int32, (SEQ, LANES), 1)
    even = (lane & 1) == 0
    low = lane < DK
    other_half = pltpu.roll(table[...], DK, 1)
    cosine = jnp.where(low, table[...], other_half)
    sine = jnp.where(low, other_half, table[...])
    gap = (
        lax.broadcasted_iota(jnp.int32, (SEQ, SEQ), 0)
        - lax.broadcasted_iota(jnp.int32, (SEQ, SEQ), 1)
    ).astype(F32)
    for who, (owner, ref) in enumerate(((c, mine), (1 - c, other))):
        terms = ref[NF * M_ROWS : NF * M_ROWS + 16].astype(F32)
        head_gain = terms[0:1] + terms[1:2] + terms[2:3]
        mask = jnp.where(gap >= 0.0, jnp.exp(jnp.maximum(gap, 0.0) * rates[2 * y + owner]), 0.0)
        for i in range(rows // SEQ):
            at = slice(i * SEQ, (i + 1) * SEQ)
            scale = scales[at, :]
            both = narrow[at, who * LANES : (who + 1) * LANES] * scale
            both = both.astype(BF).astype(F32)
            values = (wide[at, who * 256 : who * 256 + LANES] * scale).astype(BF)
            gate = (wide[at, who * 256 + LANES : (who + 1) * 256] * scale).astype(BF).astype(F32)
            swapped = jnp.where(even, pltpu.roll(both, LANES - 1, 1), pltpu.roll(both, 1, 1))
            turned = both * cosine + swapped * sine
            query = jnp.where(low, turned, 0.0)
            key = pltpu.roll(turned, DK, 1) * DK ** (-0.5)
            scores = lax.dot_general(
                query.astype(BF), key.astype(BF), TRANSPOSED, preferred_element_type=F32
            )
            retained = jnp.dot((scores * mask).astype(BF), values, preferred_element_type=F32)
            center = jnp.mean(retained, axis=-1, keepdims=True)
            off = retained - center
            spread = jnp.mean(off * off, axis=-1, keepdims=True)
            grouped = off * lax.rsqrt(spread + EPS) * head_gain
            mixed[at, who * DV : (who + 1) * DV] = (grouped * jax.nn.silu(gate)).astype(BF)


def mixer(place, rates, gain, table, xs, mine, other):
    rows = xs[0].shape[0]
    return pl.pallas_call(
        mixer_body,
        out_shape=[jax.ShapeDtypeStruct((rows, 2 * DV), BF), jax.ShapeDtypeStruct((rows, D), BF)],
        in_specs=[SM, SM] + [VM] * 8,
        out_specs=[VM, VM],
        scratch_shapes=[
            pltpu.VMEM((rows, D), BF),
            pltpu.VMEM((rows, LANES), F32),
            pltpu.VMEM((rows, 256), F32),
            pltpu.VMEM((rows, 512), F32),
        ],
        compiler_params=pltpu.CompilerParams(vmem_limit_bytes=20 * 2**20),
        cost_estimate=pl.CostEstimate(
            flops=2 * rows * D * 768, bytes_accessed=5 * 2**20, transcendentals=0
        ),
        name="mixer",
    )(place, rates, gain, table, *xs, mine, other)


PER_CORE = 704
HIDDEN = 2 * PER_CORE
UNIT = 64
PAIRS = 5
MOVED = 256
KEPT = PER_CORE - MOVED
B_ROWS = HIDDEN + MOVED


def quads(layout, mine, other):
    flat = []
    for ref, twin, (outer, entries) in zip(mine, other, layout):
        flat += [((ref, twin, entry), outer) for entry in range(len(entries))]
    for k in range(0, NF, 4):
        yield [entry for entry, _ in flat[k : k + 4]], flat[k][1]


def ffn_body(place, gain, whole, *refs):
    nb, na = len(B_LAYOUT), len(A_LAYOUT)
    mixes, refs = refs[0:4], refs[4:]
    b_mine, b_other, refs = refs[:nb], refs[nb : 2 * nb], refs[2 * nb :]
    a_mine, a_other, refs = refs[:na], refs[na : 2 * na], refs[2 * na :]
    own, *outs = refs[:7]
    resid, mixed, acts, hidden, shares, scales, squares = refs[7:]
    y, z, x = place[0], place[2], place[3]
    rows = whole.shape[0]
    for d, ref in enumerate(mixes):
        mixed[:, d * 256 : (d + 1) * 256] = ref[...]

    def columns(group, segments):
        return jnp.concatenate(
            [
                jnp.concatenate(
                    [ref[entry, at, :] for at in segments for ref in (mine, other)], axis=0
                )
                for mine, other, entry in group
            ],
            axis=1,
        )

    for group, outer in quads(A_LAYOUT, a_mine, a_other):
        wide = columns(group, [slice(KEPT + k * DV, KEPT + (k + 1) * DV) for k in range(4)])
        share = jnp.dot(mixed[...], wide, preferred_element_type=F32)
        for e, inner in enumerate(OFFSETS):
            at = lanes(((z + outer) & 3) * 4 + ((x + inner) & 3))
            rounded = (
                whole[:, at].astype(F32) + share[:, e * LANES : (e + 1) * LANES]
            ).astype(BF)
            resid[:, at] = rounded
            floats = rounded.astype(F32)
            k = e * 4 + OFFSETS.index(outer)
            acts[:, k * LANES : (k + 1) * LANES] = (floats * gain[:, at]).astype(BF)
            if e == 0 and outer == 0:
                squares[...] = floats * floats
            else:
                squares[...] += floats * floats

    total = jnp.sum(squares[...], axis=-1, keepdims=True)
    scales[...] = jnp.broadcast_to(lax.rsqrt(total / D + EPS), (rows, LANES))
    order = []
    for mine, other, (outer, entries) in zip(b_mine, b_other, B_LAYOUT):
        order += [(mine, other, entry) for entry in range(len(entries))]

    def multiply(j, units):
        width = units * UNIT
        gate_at = pl.ds(pl.multiple_of(j * UNIT, UNIT), width)
        up_at = pl.ds(pl.multiple_of(PER_CORE + j * UNIT, UNIT), width)
        wide = jnp.concatenate(
            [
                jnp.concatenate(
                    [ref[entry, at, :] for at in (gate_at, up_at) for ref in (mine, other)], axis=0
                )
                for mine, other, entry in order
            ],
            axis=1,
        )
        return lax.dot_general(acts[...], wide, TRANSPOSED, preferred_element_type=F32)

    def expand(i, carry):
        both = multiply(2 * i, 2)
        for k in range(2):
            gate = both[:, k * LANES : (k + 1) * LANES] * scales[...]
            up = both[:, 256 + k * LANES : 256 + (k + 1) * LANES] * scales[...]
            hidden[:, lanes(2 * i + k)] = (jax.nn.silu(gate) * up).astype(BF)
        return carry

    lax.fori_loop(0, PAIRS, expand, 0)
    both = multiply(2 * PAIRS, 1)
    gate, up = both[:, :LANES] * scales[...], both[:, LANES:] * scales[...]
    hidden[:, PAIRS * 256 :] = (jax.nn.silu(gate) * up).astype(BF)

    there = MOVED // (2 * UNIT)
    moved = [slice(HIDDEN + 2 * UNIT * i, HIDDEN + 2 * UNIT * (i + 1)) for i in range(there)]
    segments = [slice(2 * UNIT * i, 2 * UNIT * (i + 1)) for i in range(PAIRS - there)]
    segments.append(slice(2 * UNIT * (PAIRS - there), KEPT))
    for p, (group, outer) in enumerate(quads(A_LAYOUT, a_mine, a_other)):
        twins = [order[e * 4 + p] for e in range(4)]
        wide = jnp.concatenate([columns(twins, moved), columns(group, segments)], axis=0)
        part = jnp.dot(hidden[...], wide, preferred_element_type=F32).astype(BF)
        for e, inner in enumerate(OFFSETS):
            shares[(z + outer) & 3, :, lanes((x + inner) & 3)] = part[:, e * LANES : (e + 1) * LANES]

    half = rows // 2
    for (offset, first), out in zip(PIECES, outs):
        out[...] = shares[(y + offset) & 3, first * half : (first + 1) * half]
    mine = pl.ds(pl.multiple_of(y * 512, 512), 512)
    own[...] = resid[:, mine].astype(F32) + shares[y].astype(F32)


def feed_forward(place, gain, whole, mixes, b_both, a_both):
    rows = whole.shape[0]
    weights = [*b_both[0], *b_both[1], *a_both[0], *a_both[1]]
    return pl.pallas_call(
        ffn_body,
        out_shape=[jax.ShapeDtypeStruct((rows, 512), F32)]
        + [jax.ShapeDtypeStruct((rows // 2, 512), BF)] * 6,
        in_specs=[SM] + [VM] * (6 + len(weights)),
        out_specs=[VM] * 7,
        scratch_shapes=[
            pltpu.VMEM((rows, D), BF),
            pltpu.VMEM((rows, HEADS * DV), BF),
            pltpu.VMEM((rows, D), BF),
            pltpu.VMEM((rows, HIDDEN), BF),
            pltpu.VMEM((4, rows, 512), BF),
            pltpu.VMEM((rows, LANES), F32),
            pltpu.VMEM((rows, LANES), F32),
        ],
        compiler_params=pltpu.CompilerParams(vmem_limit_bytes=VMEM_LIMIT),
        cost_estimate=pl.CostEstimate(
            flops=6 * rows * D * HIDDEN, bytes_accessed=24 * 2**20, transcendentals=0
        ),
        name="ffn",
    )(place, gain, whole, *mixes, *weights)


PIECES = ((2, 0), (2, 1), (1, 0), (1, 1), (-1, 0), (-1, 1))
B_LAYOUT = DIRECT
A_LAYOUT = DIRECT
VMEM_LIMIT = 20 * 2**20


def join_body(place, tokens, received, own, sem):
    half, cols = received.shape
    c = place[1]
    copy = pltpu.make_async_copy(
        tokens.at[pl.ds(pl.multiple_of(c * half, half), half)],
        own.at[:, pl.ds(pl.multiple_of(c * cols, cols), cols)],
        sem,
    )
    copy.start()
    own[:, pl.ds(pl.multiple_of((1 - c) * cols, cols), cols)] = received[...]
    copy.wait()


def join(place, tokens, received):
    half, cols = received.shape
    return pl.pallas_call(
        join_body,
        out_shape=jax.ShapeDtypeStruct((half, 2 * cols), BF),
        in_specs=[SM, FAR, VM],
        out_specs=VM,
        scratch_shapes=[pltpu.SemaphoreType.DMA],
        compiler_params=pltpu.CompilerParams(vmem_limit_bytes=4 * 2**20),
        name="join",
    )(place, tokens, received)


def stack(pieces, parts):
    total = sum(rows for _, _, rows in parts(0))

    def body(*refs):
        *ins, out = refs
        for k in range(4):
            row = 0
            for source, first, rows in parts(k):
                out[k, row : row + rows, :] = ins[source][first : first + rows, :]
                row += rows

    return pl.pallas_call(
        body,
        out_shape=jax.ShapeDtypeStruct((4, total, LANES), BF),
        in_specs=[VM] * len(pieces),
        out_specs=VM,
        compiler_params=pltpu.CompilerParams(vmem_limit_bytes=4 * 2**20),
    )(*pieces)


def merge_mixer_body(gain, *refs):
    *pieces, out = refs
    for k in range(NF):
        out[k * M_ROWS : (k + 1) * M_ROWS, :] = pieces[k // 4][k % 4]
    rest = gain[...]
    terms = []
    for _ in range(3):
        terms.append(rest.astype(BF))
        rest = rest - terms[-1].astype(F32)
    terms.append(jnp.zeros((13, LANES), BF))
    out[NF * M_ROWS :, :] = jnp.concatenate([t.astype(F32) for t in terms], axis=0).astype(BF)


def merge_mixer(gain, pieces):
    return pl.pallas_call(
        merge_mixer_body,
        out_shape=jax.ShapeDtypeStruct((NF * M_ROWS + 16, LANES), BF),
        in_specs=[VM] * 5,
        out_specs=VM,
        compiler_params=pltpu.CompilerParams(vmem_limit_bytes=4 * 2**20),
        name="merge_mixer",
    )(gain, *pieces)


def merge_halves_body(first, second, out):
    out[0:2] = first[...]
    out[2:4] = second[...]


def merge_halves(first, second):
    return pl.pallas_call(
        merge_halves_body,
        out_shape=jax.ShapeDtypeStruct((4, *first.shape[1:]), BF),
        in_specs=[VM] * 2,
        out_specs=VM,
        compiler_params=pltpu.CompilerParams(vmem_limit_bytes=4 * 2**20),
    )(first, second)


def halves_in_order(c, own, received, axis):
    lower = jnp.where(c == 0, own, received)
    upper = jnp.where(c == 0, received, own)
    return jnp.concatenate([lower, upper], axis=axis)


def rotation_table():
    frequency = ROPE_BASE ** (-np.linspace(0.0, 1.0, DK // 2))
    angles = np.repeat(np.arange(SEQ)[:, None] * frequency[None, :], 2, axis=1)
    signs = np.tile([-1.0, 1.0], DK // 2)[None, :]
    return np.concatenate([np.cos(angles), np.sin(angles) * signs], axis=1).astype(np.float32)


def per_device(
    tokens,
    mix_gain,
    query_weight,
    key_weight,
    value_weight,
    gate_weight,
    out_weight,
    head_gain,
    ffn_gain,
    ffn_gate,
    ffn_up,
    ffn_down,
):
    y, c, z, x = (lax.axis_index(n) for n in ("y", "c", "z", "x"))
    place = jnp.stack([y, c, z, x]).astype(jnp.int32)
    table = jnp.asarray(rotation_table())
    rates = jnp.asarray(np.log1p(-np.exp2(-5.0 - 4.0 * np.arange(HEADS) / (HEADS - 1))), F32)
    half_cols = tokens.shape[1]

    b_pack = jnp.concatenate([ffn_gate.T, ffn_up.T, ffn_down[:MOVED]], axis=0)
    half = tokens.shape[0] // 2
    given = lax.dynamic_slice_in_dim(tokens, (1 - c) * half, half, 0)
    x_pack = jnp.concatenate([query_weight.T, key_weight.T, value_weight, gate_weight], axis=0)
    x_pack = jnp.concatenate([ffn_down[MOVED:], lax.optimization_barrier(x_pack), out_weight], axis=0)
    own = join(place, tokens, core_swap(given))

    column = stack(gather_direct(b_pack, Z_AXIS), lambda k: [(k, 0, B_ROWS)])
    b_mine = gather_relayed(column, X_AXIS)
    b_other = [core_swap(p) for p in b_mine]

    row = gather_direct(x_pack, X_AXIS)
    m_mine = gather_direct(stack(row, lambda k: [(k, KEPT, M_ROWS)]), Z_AXIS)
    m_mine = merge_mixer(head_gain, m_mine)
    m_other = core_swap(m_mine)

    heads = stack(row, lambda k: [(k, KEPT + M_ROWS, DV)]).reshape(4 * DV, LANES)
    heads = gather_direct(heads, Y_AXIS)
    row = stack([*row, *heads], lambda k: [(k, 0, KEPT)] + [(4 + d, k * DV, DV) for d in range(4)])
    a_mine = gather_relayed(row, Z_AXIS)
    a_other = [core_swap(p) for p in a_mine]

    xs = gather_direct(own, Y_AXIS)
    mixed, whole = mixer(
        place, rates, mix_gain[None], table, xs, m_mine, m_other
    )
    mixes = gather_direct(mixed, Y_AXIS)
    total, far_top, far_low, up_top, up_low, down_top, down_low = feed_forward(
        place, ffn_gain[None], whole, mixes, (b_mine, b_other), (a_mine, a_other)
    )
    far_top = from_offset(far_top, Y_AXIS, -1)
    far_low = from_offset(far_low, Y_AXIS, 1)
    near_low = from_offset(up_low, Y_AXIS, -1)
    near_top = from_offset(down_top, Y_AXIS, 1)
    up_top = (up_top.astype(F32) + far_top.astype(F32)).astype(BF)
    down_low = (down_low.astype(F32) + far_low.astype(F32)).astype(BF)
    top = near_top.astype(F32) + from_offset(up_top, Y_AXIS, -1).astype(F32)
    low = near_low.astype(F32) + from_offset(down_low, Y_AXIS, 1).astype(F32)
    total = total + jnp.concatenate([top, low], axis=0)
    done = total.astype(BF)
    kept = lax.dynamic_slice_in_dim(done, c * half_cols, half_cols, 1)
    given = lax.dynamic_slice_in_dim(done, (1 - c) * half_cols, half_cols, 1)
    return halves_in_order(c, kept, core_swap(given), 0)


def solution(mesh):
    finer = Mesh(mesh.devices.reshape(2, 4, 4, 4, 2), ("rep", "z", "x", "y", "c"))
    fs, tp = ("z", "x"), ("y", "c")
    rows = ("rep", "z", "x")
    placed = (
        P(rows, tp), P(), P(fs, tp), P(fs, tp), P(fs, tp), P(fs, tp), P(tp, fs), P(tp, None), P(),
        P(fs, tp), P(fs, tp), P(tp, fs),
    )
    return jax.shard_map(
        per_device, mesh=finer, in_specs=placed, out_specs=P(rows, tp), check_vma=False
    )
```
